128 devices in a mesh: sp: 16 (over z, y), tp: 8 (over x, core).
Axes of the slice: x: 4, y: 4, z: 4, core: 2. Of those that a mesh axis runs over, the one named last changes fastest.
Arguments:
- resid: bfloat16 [16384, 2048], P(('sp', 'tp')), may hold values from -6 to 6
- query_nope: bfloat16 [16384, 2048], P('sp', 'tp'), may hold values from -18 to 18
- query_rope: bfloat16 [16384, 1024], P('sp', 'tp'), may hold values from -300 to 300
- latent: bfloat16 [16384, 256], P('sp'), may hold values from -6 to 6
- key_rope: bfloat16 [16384, 64], P('sp'), may hold values from -6 to 6
- latent_gain: float32 [256], replicated, may hold values from 0.1 to 1.9
- w_key: bfloat16 [256, 2048], P(None, 'tp'), may hold values from -0.375 to 0.375
- w_value: bfloat16 [256, 2048], P(None, 'tp'), may hold values from -0.375 to 0.375
- w_out: bfloat16 [2048, 2048], P('tp'), may hold values from -0.125 to 0.125
- mix_gain: float32 [2048], replicated, may hold values from 0.1 to 1.9
- w_gate: bfloat16 [2048, 5632], P('sp', 'tp'), may hold values from -0.125 to 0.125
- w_up: bfloat16 [2048, 5632], P('sp', 'tp'), may hold values from -0.125 to 0.125
- w_down: bfloat16 [2048, 5632], P('sp', 'tp'), may hold values from -0.078125 to 0.078125
Outputs:
- layer_out: bfloat16 [16384, 2048], P(('sp', 'tp'))
The draws below stay inside these ranges and needn't reach their ends.
All inputs are finite; a program needn't handle non-finite values.
Results may differ from the reference program's by a relative error of at most 0.0095.
Values may be sent and summed in bfloat16 or wider, within the bound.
No kernel may reach another device: no remote copies, remote signals or barrier semaphores. Data moves between devices by JAX's collectives and lax.ppermute only.
A program may use at most 128 MiB of HBM per device.

```python
import jax
import jax.numpy as jnp
from jax import lax

D = 2048
HEADS = 16
NOPE = 128
ROPE = 64
VDIM = 128
RANK = 256
FF = 5632
TOK_DEV = 1024
TOKENS = 16384
N_SP = 16
N_TP = 8


def rope_pair(key):
    base_key = jax.random.fold_in(key, 11)
    key_one, key_two = jax.random.split(base_key, 2)
    key_part = jax.random.truncated_normal(key_one, -5.0, 5.0, (TOKENS, ROPE), jnp.float32)
    query_part = 3.0 * jax.random.truncated_normal(key_two, -5.0, 5.0, (TOKENS, HEADS * ROPE), jnp.float32)
    return (key_part, query_part)


def draw_query_rope(key, part):
    return rope_pair(key)[1].astype(jnp.bfloat16)


def draw_key_rope(key, part):
    return rope_pair(key)[0].astype(jnp.bfloat16)


def block_levels(key, dims, cuts, least, top_value):
    def one(position, blocks):
        heights = jax.random.uniform(jax.random.fold_in(jax.random.fold_in(key, 6), position), (blocks,), jnp.float32, least / len(cuts), top_value / len(cuts))
        return jnp.repeat(jnp.exp(heights), dims[position] // blocks).reshape((-1,) + (1,) * (len(dims) - position - 1))

    factor_of = one(*cuts[0])
    for cut in cuts[1:]:
        factor_of = factor_of * one(*cut)
    return factor_of


def bell_draw(stream_key, dims, spread, reach, cuts=(), held_as=jnp.bfloat16):
    loudness = block_levels(stream_key, dims, cuts, -0.22, 0.18) if cuts else 1.0
    result = jax.random.normal(stream_key, dims, jnp.float32) * spread * loudness
    return jnp.minimum(jnp.maximum(result, -reach), reach).astype(held_as)


def setup_inputs(seed: int = 0) -> dict:
    splits = jax.random.split(jax.random.key(seed), 14)
    resid = bell_draw(splits[0], (TOKENS, D), 1.0, 6.0, ((0, 128),))
    query_nope = bell_draw(splits[1], (TOKENS, HEADS * NOPE), 3.0, 18.0, ((0, 16), (1, 8)))
    query_rope = draw_query_rope(jax.random.fold_in(splits[13], 71), 0)
    latent = bell_draw(splits[3], (TOKENS, RANK), 1.0, 6.0, ((0, 16),))
    key_rope = draw_key_rope(jax.random.fold_in(splits[13], 71), 0)
    latent_gain = jnp.clip(1.0 + 0.18 * jax.random.normal(splits[5], (RANK,), jnp.float32), 0.1, 1.9)
    w_key = bell_draw(splits[6], (RANK, HEADS * NOPE), RANK ** -0.5, 0.375, ((1, 8),))
    w_value = bell_draw(splits[7], (RANK, HEADS * VDIM), RANK ** -0.5, 0.375, ((1, 8),))
    w_out = bell_draw(splits[8], (HEADS * VDIM, D), (HEADS * VDIM) ** -0.5, 0.125, ((0, 8),))
    mix_gain = jnp.clip(1.0 + 0.18 * jax.random.normal(splits[9], (D,), jnp.float32), 0.1, 1.9)
    w_gate = bell_draw(splits[10], (D, FF), D ** -0.5, 0.125, ((0, 16), (1, 8)))
    w_up = bell_draw(splits[11], (D, FF), D ** -0.5, 0.125, ((0, 16), (1, 8)))
    w_down = bell_draw(splits[12], (D, FF), FF ** -0.5, 0.078125, ((0, 16), (1, 8)))
    return {"resid": resid, "query_nope": query_nope, "query_rope": query_rope, "latent": latent, "key_rope": key_rope, "latent_gain": latent_gain, "w_key": w_key, "w_value": w_value, "w_out": w_out, "mix_gain": mix_gain, "w_gate": w_gate, "w_up": w_up, "w_down": w_down}


norm_eps = 1e-06
masked_score = -1e+30
theta_base = 10000.0

def rotate(values_in, angle):
    half_width = values_in.shape[-1] // 2
    front_half = values_in[..., :half_width]
    back_half = values_in[..., half_width:]
    cosine = jnp.cos(angle)
    sine_part = jnp.sin(angle)
    return jnp.concatenate([front_half * cosine - back_half * sine_part, back_half * cosine + front_half * sine_part], axis=-1)

def angles(positions, full_width):
    half_width = full_width // 2
    frequency = theta_base ** (-2.0 * jnp.arange(half_width).astype(jnp.float32) / full_width)
    return positions[:, None] * frequency[None, :]

def rms_scale(values_in, gain):
    return values_in * lax.rsqrt(lax.optimization_barrier(jnp.mean(values_in * values_in, axis=-1, keepdims=True)) + norm_eps) * gain

def reference(resid, query_nope, query_rope, latent, key_rope, latent_gain, w_key, w_value, w_out, mix_gain, w_gate, w_up, w_down):
    positions = jnp.arange(TOKENS).astype(jnp.float32)
    angle = angles(positions, ROPE)
    latent_normed = rms_scale(latent.astype(jnp.float32), latent_gain).astype(jnp.bfloat16)
    head_keys = jnp.dot(latent_normed, w_key, preferred_element_type=jnp.float32).astype(jnp.bfloat16)
    head_values = jnp.dot(latent_normed, w_value, preferred_element_type=jnp.float32).astype(jnp.bfloat16)
    key_rotated = rotate(key_rope.astype(jnp.float32), angle).astype(jnp.bfloat16)
    query_rotated = rotate(query_rope.astype(jnp.float32).reshape(TOKENS, HEADS, ROPE), angle[:, None, :]).astype(jnp.bfloat16)
    by_head_nope = jnp.transpose(query_nope.reshape(TOKENS, HEADS, NOPE), (1, 0, 2))
    by_head_rope = jnp.transpose(query_rotated, (1, 0, 2))
    by_head_keys = jnp.transpose(head_keys.reshape(TOKENS, HEADS, NOPE), (1, 0, 2))
    by_head_values = jnp.transpose(head_values.reshape(TOKENS, HEADS, VDIM), (1, 0, 2))
    score_scale = (NOPE + ROPE) ** (-0.5)
    key_positions = jnp.arange(TOKENS).astype(jnp.int32)

    def one_head(operands):
        nope_q, rope_q, keys_h, values_h = operands

        def one_block(block_index):
            first_row = block_index * TOK_DEV
            query_part = lax.dynamic_slice_in_dim(nope_q, first_row, TOK_DEV, 0)
            rope_part = lax.dynamic_slice_in_dim(rope_q, first_row, TOK_DEV, 0)
            scores = jnp.dot(query_part, keys_h.T, preferred_element_type=jnp.float32)
            scores = (scores + jnp.dot(rope_part, key_rotated.T, preferred_element_type=jnp.float32)) * score_scale
            query_rows = first_row + jnp.arange(TOK_DEV).astype(jnp.int32)
            causal = key_positions[None, :] <= query_rows[:, None]
            scores = jnp.where(causal, scores, masked_score)
            row_max = lax.optimization_barrier(jnp.max(scores, axis=-1, keepdims=True))
            weights = jnp.where(causal, jnp.exp(scores - row_max), 0.0)
            weight_sum = lax.optimization_barrier(jnp.sum(weights, axis=-1, keepdims=True))
            mixed = jnp.dot(weights.astype(jnp.bfloat16), values_h, preferred_element_type=jnp.float32)
            return (mixed / weight_sum).astype(jnp.bfloat16)
        return lax.map(one_block, jnp.arange(N_SP).astype(jnp.int32))
    head_out = lax.map(one_head, (by_head_nope, by_head_rope, by_head_keys, by_head_values))
    head_out = head_out.reshape(HEADS, TOKENS, VDIM)
    group_heads = HEADS // N_TP
    out_heads = w_out.reshape(HEADS, VDIM, D)
    attention_proj = jnp.zeros((TOKENS, D), jnp.float32)
    for group_index in range(N_TP):
        picked = slice(group_index * group_heads, (group_index + 1) * group_heads)
        partial_sum = jnp.einsum('htv,hvd->td', head_out[picked].astype(jnp.float32), out_heads[picked].astype(jnp.float32))
        attention_proj = attention_proj + lax.optimization_barrier(partial_sum.astype(jnp.bfloat16)).astype(jnp.float32)
    stream = resid.astype(jnp.float32) + attention_proj
    normed = rms_scale(stream, mix_gain).astype(jnp.bfloat16)
    group_units = FF // N_TP
    mixer_out = jnp.zeros((TOKENS, D), jnp.float32)
    for group_index in range(N_TP):
        columns = slice(group_index * group_units, (group_index + 1) * group_units)
        gate_value = jnp.dot(normed, w_gate[:, columns], preferred_element_type=jnp.float32)
        upward = jnp.dot(normed, w_up[:, columns], preferred_element_type=jnp.float32)
        hidden = (jax.nn.silu(gate_value) * upward).astype(jnp.bfloat16)
        partial_sum = jnp.dot(hidden, w_down[:, columns].T, preferred_element_type=jnp.float32)
        mixer_out = mixer_out + lax.optimization_barrier(partial_sum.astype(jnp.bfloat16)).astype(jnp.float32)
    return (stream + 0.5 * mixer_out).astype(jnp.bfloat16)
```

```python
import functools

import jax
import jax.numpy as jnp
from jax import lax
from jax.experimental import pallas as pl
from jax.experimental.pallas import tpu as pltpu
from jax.sharding import PartitionSpec as P

NOPE = 128
ROPE = 64
VDIM = 128
TILE = 256
LOG2E = 1.4426950408889634

norm_eps = 1e-06
masked_score = -1e30
theta_base = 10000.0


def rotate(values_in, angle):
    half_width = values_in.shape[-1] // 2
    front_half = values_in[..., :half_width]
    back_half = values_in[..., half_width:]
    cosine = jnp.cos(angle)
    sine_part = jnp.sin(angle)
    return jnp.concatenate(
        [front_half * cosine - back_half * sine_part, back_half * cosine + front_half * sine_part],
        axis=-1,
    )


def angles(positions, full_width):
    half_width = full_width // 2
    frequency = theta_base ** (-2.0 * jnp.arange(half_width).astype(jnp.float32) / full_width)
    return positions[:, None] * frequency[None, :]


def rms_scale(values_in, gain):
    return (
        values_in
        * lax.rsqrt(jnp.mean(values_in * values_in, axis=-1, keepdims=True) + norm_eps)
        * gain
    )


def attention_kernel(rows, lo_ref, block_ref, qa_ref, qb_ref, wkv_ref, out_ref, k_ref, v_ref, m_ref, acc_ref):
    step = pl.program_id(0)
    steps = pl.num_programs(0)
    low = lo_ref[0]
    high = steps - 1 - low
    tiles = rows // TILE
    scale = (NOPE + ROPE) ** (-0.5) * LOG2E

    @pl.when(step == 0)
    def _():
        m_ref[...] = jnp.full(m_ref.shape, masked_score, jnp.float32)
        acc_ref[...] = jnp.zeros(acc_ref.shape, jnp.float32)
        v_ref[:, VDIM:] = jnp.ones((rows, VDIM), jnp.bfloat16)

    def scores(row_start, part):
        q_ref = qa_ref if part % 2 == 0 else qb_ref
        return lax.dot_general(
            q_ref[pl.ds(row_start, TILE), :],
            k_ref[part * TILE : (part + 1) * TILE, :],
            (((1,), (1,)), ((), ())),
            preferred_element_type=jnp.float32,
        )

    def fold(row_start, parts, diagonal):
        s = [scores(row_start, part) * scale for part in range(parts)]
        if diagonal:
            row = lax.broadcasted_iota(jnp.int32, (TILE, TILE), 0)
            col = lax.broadcasted_iota(jnp.int32, (TILE, TILE), 1)
            s[-1] = jnp.where(col <= row, s[-1], masked_score)
        top = s[0]
        for other in s[1:]:
            top = jnp.maximum(top, other)
        old_max = m_ref[pl.ds(row_start, TILE), :]
        new_max = jnp.maximum(old_max, jnp.max(top, axis=-1, keepdims=True))
        factor = jnp.exp2(old_max - new_max)
        wide_max = jnp.concatenate([new_max, new_max], axis=1)
        total = jnp.concatenate([factor, factor], axis=1) * acc_ref[pl.ds(row_start, TILE), :]
        for part in range(parts):
            weights = jnp.exp2(s[part] - wide_max).astype(jnp.bfloat16)
            total = total + jnp.dot(
                weights,
                v_ref[part * TILE : (part + 1) * TILE, :],
                preferred_element_type=jnp.float32,
            )
        m_ref[pl.ds(row_start, TILE), :] = new_max
        acc_ref[pl.ds(row_start, TILE), :] = total

    @pl.when(step <= high)
    def _():
        expanded = jnp.dot(
            block_ref[0, :rows, :], wkv_ref[...], preferred_element_type=jnp.float32
        ).astype(jnp.bfloat16)
        k_ref[:, :NOPE] = expanded[:, :NOPE]
        v_ref[:, :VDIM] = expanded[:, NOPE:]
        for part in range(tiles):
            k_ref[part * TILE : (part + 1) * TILE, NOPE:] = block_ref[
                0, rows:, (part // 2) * 128 : (part // 2 + 1) * 128
            ]

        first = jnp.where(step < low, 0, 1)
        last = jnp.where(step < high, 2, 1)

        def whole(group, carry):
            base = group * rows
            for tile in range(tiles):
                fold(pl.multiple_of(base + tile * TILE, TILE), tiles, False)
            return carry

        lax.fori_loop(first, last, whole, 0)

        @pl.when((step == low) | (step == high))
        def _():
            base = jnp.where(step == low, 0, rows)
            for tile in range(tiles):
                fold(pl.multiple_of(base + tile * TILE, TILE), tile + 1, True)

    @pl.when(step == steps - 1)
    def _():
        out_ref[...] = (acc_ref[:, :VDIM] / acc_ref[:, VDIM:]).astype(jnp.bfloat16)


def attention(low, blocks, query_a, query_b, w_kv):
    count, packed_rows, width = blocks.shape
    rows = query_a.shape[0] // 2
    return pl.pallas_call(
        functools.partial(attention_kernel, rows),
        grid_spec=pltpu.PrefetchScalarGridSpec(
            num_scalar_prefetch=1,
            grid=(count,),
            in_specs=[
                pl.BlockSpec((1, packed_rows, width), lambda i, lo: (jnp.minimum(i, count - 1 - lo[0]), 0, 0)),
                pl.BlockSpec(query_a.shape, lambda i, lo: (0, 0)),
                pl.BlockSpec(query_b.shape, lambda i, lo: (0, 0)),
                pl.BlockSpec(w_kv.shape, lambda i, lo: (0, 0)),
            ],
            out_specs=pl.BlockSpec((2 * rows, VDIM), lambda i, lo: (0, 0)),
            scratch_shapes=[
                pltpu.VMEM((rows, NOPE + 128), jnp.bfloat16),
                pltpu.VMEM((rows, 2 * VDIM), jnp.bfloat16),
                pltpu.VMEM((2 * rows, 128), jnp.float32),
                pltpu.VMEM((2 * rows, 2 * VDIM), jnp.float32),
            ],
        ),
        out_shape=jax.ShapeDtypeStruct((2 * rows, VDIM), jnp.bfloat16),
        compiler_params=pltpu.CompilerParams(dimension_semantics=("arbitrary",)),
        cost_estimate=pl.CostEstimate(
            flops=17 * rows * rows * 1024, bytes_accessed=blocks.size * 2, transcendentals=17 * rows * rows
        ),
        name="attention",
    )(low, blocks, query_a, query_b, w_kv)


def on_device(
    resid,
    query_nope,
    query_rope,
    latent,
    key_rope,
    latent_gain,
    w_key,
    w_value,
    w_out,
    mix_gain,
    w_gate,
    w_up,
    w_down,
):
    n_sp = lax.axis_size("sp")
    n_tp = lax.axis_size("tp")
    rows = query_nope.shape[0]
    here = lax.axis_index("sp")
    upper = here >= n_sp // 2
    first_row = here * rows
    angle = angles((first_row + jnp.arange(rows, dtype=jnp.int32)).astype(jnp.float32), ROPE)

    latent_normed = rms_scale(latent.astype(jnp.float32), latent_gain).astype(jnp.bfloat16)
    key_rotated = rotate(key_rope.astype(jnp.float32), angle).astype(jnp.bfloat16)
    packed_rope = jnp.concatenate(jnp.split(key_rotated, 4, axis=0), axis=1)
    own_block = jnp.concatenate([latent_normed, packed_rope], axis=0)
    blocks = lax.all_gather(own_block, "sp", axis=0, tiled=False)
    weights_full = lax.all_gather(
        jnp.concatenate([w_gate, w_up, w_down], axis=1), "sp", axis=0, tiled=True
    )
    out_full = lax.all_gather(w_out, "tp", axis=0, tiled=True)

    rope_query = rotate(
        query_rope.astype(jnp.float32).reshape(rows, 2, ROPE), angle[:, None, :]
    ).astype(jnp.bfloat16)
    blank = jnp.zeros((rows, ROPE), jnp.bfloat16)
    by_head = [
        jnp.concatenate([query_nope[:, h * NOPE : (h + 1) * NOPE], rope_query[:, h], blank], axis=1)
        for h in range(2)
    ]
    kept = jnp.where(upper, by_head[1], by_head[0])
    given = jnp.where(upper, by_head[0], by_head[1])
    partner = [(i, n_sp - 1 - i) for i in range(n_sp)]
    taken = lax.ppermute(given, "sp", partner)
    query_a = jnp.where(
        upper, jnp.concatenate([taken, kept], axis=0), jnp.concatenate([kept, taken], axis=0)
    )
    query_b = jnp.concatenate([query_a[:, :NOPE], query_a[:, NOPE + ROPE :], query_a[:, NOPE : NOPE + ROPE]], axis=1)
    w_kv = jnp.where(
        upper,
        jnp.concatenate([w_key[:, NOPE:], w_value[:, VDIM:]], axis=1),
        jnp.concatenate([w_key[:, :NOPE], w_value[:, :VDIM]], axis=1),
    )
    low = jnp.minimum(here, n_sp - 1 - here).astype(jnp.int32).reshape(1)
    head_out = attention(low, blocks, query_a, query_b, w_kv)

    groups = [
        [b * n_tp + t for b in (p, n_sp - 1 - p) for t in range(n_tp)] for p in range(n_sp // 2)
    ]
    piece = rows // n_tp
    arrived = lax.all_to_all(
        head_out.reshape(2 * n_tp, piece, VDIM),
        ("sp", "tp"),
        split_axis=0,
        concat_axis=0,
        axis_index_groups=groups,
        tiled=True,
    )
    all_heads = arrived.reshape(2, n_tp, piece, VDIM).transpose(2, 1, 0, 3).reshape(piece, 2 * n_tp * VDIM)
    attention_proj = jnp.dot(all_heads, out_full, preferred_element_type=jnp.float32)
    stream = resid.astype(jnp.float32) + attention_proj
    normed = rms_scale(stream, mix_gain).astype(jnp.bfloat16)
    row_piece = lax.all_gather(normed, "tp", axis=0, tiled=True)
    units = w_gate.shape[1]
    gate_value = jnp.dot(row_piece, weights_full[:, :units], preferred_element_type=jnp.float32)
    upward = jnp.dot(row_piece, weights_full[:, units : 2 * units], preferred_element_type=jnp.float32)
    hidden = (jax.nn.silu(gate_value) * upward).astype(jnp.bfloat16)
    down_term = lax.dot_general(
        hidden, weights_full[:, 2 * units :], (((1,), (1,)), ((), ())), preferred_element_type=jnp.float32
    )
    mixer_out = lax.psum_scatter(
        down_term.astype(jnp.bfloat16), "tp", scatter_dimension=0, tiled=True
    ).astype(jnp.float32)
    return (stream + 0.5 * mixer_out).astype(jnp.bfloat16)


def solution(mesh):
    return jax.shard_map(
        on_device,
        mesh=mesh,
        in_specs=(
            P(("sp", "tp"), None),
            P("sp", "tp"),
            P("sp", "tp"),
            P("sp", None),
            P("sp", None),
            P(),
            P(None, "tp"),
            P(None, "tp"),
            P("tp", None),
            P(),
            P("sp", "tp"),
            P("sp", "tp"),
            P("sp", "tp"),
        ),
        out_specs=P(("sp", "tp"), None),
        check_vma=False,
    )
```

```python
import functools

import jax
import jax.numpy as jnp
from jax import lax
from jax.experimental import pallas as pl
from jax.experimental.pallas import tpu as pltpu
from jax.sharding import PartitionSpec as P

NOPE = 128
ROPE = 64
VDIM = 128
TILE = 256
LOG2E = 1.4426950408889634

norm_eps = 1e-06
masked_score = -1e30
theta_base = 10000.0


def rotate(values_in, angle):
    half_width = values_in.shape[-1] // 2
    front_half = values_in[..., :half_width]
    back_half = values_in[..., half_width:]
    cosine = jnp.cos(angle)
    sine_part = jnp.sin(angle)
    return jnp.concatenate(
        [front_half * cosine - back_half * sine_part, back_half * cosine + front_half * sine_part],
        axis=-1,
    )


def angles(positions, full_width):
    half_width = full_width // 2
    frequency = theta_base ** (-2.0 * jnp.arange(half_width).astype(jnp.float32) / full_width)
    return positions[:, None] * frequency[None, :]


def rms_scale(values_in, gain):
    return (
        values_in
        * lax.rsqrt(jnp.mean(values_in * values_in, axis=-1, keepdims=True) + norm_eps)
        * gain
    )


def attention_kernel(rows, place_ref, mine_ref, theirs_ref, qa_ref, qb_ref, wkv_ref, out_ref, k_ref, v_ref, m_ref, acc_ref):
    step = pl.program_id(0)
    steps = pl.num_programs(0)
    low = place_ref[0]
    core = place_ref[1]
    high = steps - 1 - low
    tiles = rows // TILE
    scale = (NOPE + ROPE) ** (-0.5) * LOG2E

    @pl.when(step == 0)
    def _():
        m_ref[...] = jnp.full(m_ref.shape, masked_score, jnp.float32)
        acc_ref[...] = jnp.zeros(acc_ref.shape, jnp.float32)
        v_ref[:, VDIM:] = jnp.ones((rows, VDIM), jnp.bfloat16)

    def scores(row_start, part):
        q_ref = qa_ref if part % 2 == 0 else qb_ref
        return lax.dot_general(
            q_ref[pl.ds(row_start, TILE), :],
            k_ref[part * TILE : (part + 1) * TILE, :],
            (((1,), (1,)), ((), ())),
            preferred_element_type=jnp.float32,
        )

    def fold(row_start, parts, diagonal):
        s = [scores(row_start, part) * scale for part in range(parts)]
        if diagonal:
            row = lax.broadcasted_iota(jnp.int32, (TILE, TILE), 0)
            col = lax.broadcasted_iota(jnp.int32, (TILE, TILE), 1)
            s[-1] = jnp.where(col <= row, s[-1], masked_score)
        top = s[0]
        for other in s[1:]:
            top = jnp.maximum(top, other)
        old_max = m_ref[pl.ds(row_start, TILE), :]
        new_max = jnp.maximum(old_max, jnp.max(top, axis=-1, keepdims=True))
        factor = jnp.exp2(old_max - new_max)
        wide_max = jnp.concatenate([new_max, new_max], axis=1)
        total = jnp.concatenate([factor, factor], axis=1) * acc_ref[pl.ds(row_start, TILE), :]
        for part in range(parts):
            weights = jnp.exp2(s[part] - wide_max).astype(jnp.bfloat16)
            total = total + jnp.dot(
                weights,
                v_ref[part * TILE : (part + 1) * TILE, :],
                preferred_element_type=jnp.float32,
            )
        m_ref[pl.ds(row_start, TILE), :] = new_max
        acc_ref[pl.ds(row_start, TILE), :] = total

    @pl.when(step <= high)
    def _():
        half = rows // 2
        quarter = half // 4
        for block_ref, which in ((mine_ref, core), (theirs_ref, 1 - core)):
            expanded = jnp.dot(
                block_ref[0, :half, :], wkv_ref[...], preferred_element_type=jnp.float32
            ).astype(jnp.bfloat16)
            start = pl.multiple_of(which * half, half)
            k_ref[pl.ds(start, half), :NOPE] = expanded[:, :NOPE]
            v_ref[pl.ds(start, half), :VDIM] = expanded[:, NOPE:]
            for part in range(4):
                k_ref[pl.ds(start + part * quarter, quarter), NOPE:] = block_ref[
                    0, half:, (part % 2) * 128 : (part % 2 + 1) * 128
                ]

        first = jnp.where(step < low, 0, 1)
        last = jnp.where(step < high, 2, 1)

        def whole(group, carry):
            base = group * rows
            for tile in range(tiles):
                fold(pl.multiple_of(base + tile * TILE, TILE), tiles, False)
            return carry

        lax.fori_loop(first, last, whole, 0)

        @pl.when((step == low) | (step == high))
        def _():
            base = jnp.where(step == low, 0, rows)
            for tile in range(tiles):
                fold(pl.multiple_of(base + tile * TILE, TILE), tile + 1, True)

    @pl.when(step == steps - 1)
    def _():
        out_ref[...] = (acc_ref[:, :VDIM] / acc_ref[:, VDIM:]).astype(jnp.bfloat16)


def attention(place, mine, theirs, query_a, query_b, w_kv):
    count, packed_rows, width = mine.shape
    rows = query_a.shape[0] // 2
    block_spec = pl.BlockSpec(
        (1, packed_rows, width), lambda i, place: (jnp.minimum(i, count - 1 - place[0]), 0, 0)
    )
    return pl.pallas_call(
        functools.partial(attention_kernel, rows),
        grid_spec=pltpu.PrefetchScalarGridSpec(
            num_scalar_prefetch=1,
            grid=(count,),
            in_specs=[
                block_spec,
                block_spec,
                pl.BlockSpec(query_a.shape, lambda i, place: (0, 0)),
                pl.BlockSpec(query_b.shape, lambda i, place: (0, 0)),
                pl.BlockSpec(w_kv.shape, lambda i, place: (0, 0)),
            ],
            out_specs=pl.BlockSpec((2 * rows, VDIM), lambda i, place: (0, 0)),
            scratch_shapes=[
                pltpu.VMEM((rows, NOPE + 128), jnp.bfloat16),
                pltpu.VMEM((rows, 2 * VDIM), jnp.bfloat16),
                pltpu.VMEM((2 * rows, 128), jnp.float32),
                pltpu.VMEM((2 * rows, 2 * VDIM), jnp.float32),
            ],
        ),
        out_shape=jax.ShapeDtypeStruct((2 * rows, VDIM), jnp.bfloat16),
        compiler_params=pltpu.CompilerParams(dimension_semantics=("arbitrary",)),
        cost_estimate=pl.CostEstimate(
            flops=17 * rows * rows * 1024, bytes_accessed=mine.size * 4, transcendentals=17 * rows * rows
        ),
        name="attention",
    )(place, mine, theirs, query_a, query_b, w_kv)


def project_kernel(place_ref, heads_ref, *refs):
    count = len(refs) - 4
    pieces, (resid_ref, gain_ref, stream_ref, normed_ref) = refs[:count], refs[count:]
    total = resid_ref[...].astype(jnp.float32)
    for i, piece_ref in enumerate(pieces):
        owner = place_ref[2 + i]
        heads = jnp.concatenate([heads_ref[owner], heads_ref[count + owner]], axis=1)
        total = total + jnp.dot(heads, piece_ref[...], preferred_element_type=jnp.float32)
    stream_ref[...] = total
    square = jnp.mean(total * total, axis=-1, keepdims=True)
    normed_ref[...] = (total * lax.rsqrt(square + norm_eps) * gain_ref[...]).astype(jnp.bfloat16)


def project(place, heads, pieces, resid, gain):
    rows, width = resid.shape
    return pl.pallas_call(
        project_kernel,
        grid_spec=pltpu.PrefetchScalarGridSpec(
            num_scalar_prefetch=1,
            grid=(1,),
            in_specs=[pl.BlockSpec(heads.shape, lambda i, place: (0, 0, 0))]
            + [pl.BlockSpec(p.shape, lambda i, place: (0, 0)) for p in pieces]
            + [
                pl.BlockSpec(resid.shape, lambda i, place: (0, 0)),
                pl.BlockSpec((1, width), lambda i, place: (0, 0)),
            ],
            out_specs=[pl.BlockSpec(resid.shape, lambda i, place: (0, 0))] * 2,
        ),
        out_shape=[
            jax.ShapeDtypeStruct(resid.shape, jnp.float32),
            jax.ShapeDtypeStruct(resid.shape, jnp.bfloat16),
        ],
        cost_estimate=pl.CostEstimate(
            flops=2 * rows * width * width, bytes_accessed=2 * width * width, transcendentals=0
        ),
        name="project",
    )(place, heads, *pieces, resid, gain.reshape(1, width))


def mixer_kernel(sets, units, weight_ref, *refs):
    rows_in, rows_out = refs[:sets], refs[sets : 2 * sets]
    both_ref, down_ref = refs[2 * sets :]
    step = pl.program_id(0)
    depth = weight_ref.shape[0]
    width = down_ref.shape[0]

    start = pl.multiple_of(step * depth, depth)
    x = jnp.concatenate([r[:, pl.ds(start, depth)] for r in rows_in], axis=0)
    term = jnp.dot(x, weight_ref[:, : 2 * units], preferred_element_type=jnp.float32)

    @pl.when(step == 0)
    def _():
        both_ref[...] = term

    @pl.when(step > 0)
    def _():
        both_ref[...] = both_ref[...] + term

    down_ref[pl.ds(start, depth), :] = weight_ref[:, 2 * units :]

    @pl.when(step == pl.num_programs(0) - 1)
    def _():
        gate = both_ref[:, :units]
        hidden = (gate / (1.0 + jnp.exp(-gate)) * both_ref[:, units:]).astype(jnp.bfloat16)
        out = lax.dot_general(
            hidden, down_ref[...], (((1,), (1,)), ((), ())), preferred_element_type=jnp.float32
        ).astype(jnp.bfloat16)
        rows = out.shape[0] // sets
        for i, ref in enumerate(rows_out):
            ref[...] = out[i * rows : (i + 1) * rows]


def mixer(weights, row_sets):
    rows, width = row_sets[0].shape
    units = weights.shape[1] // 3
    sets = len(row_sets)
    depth = 512
    whole = pl.BlockSpec((rows, width), lambda i: (0, 0))
    return pl.pallas_call(
        functools.partial(mixer_kernel, sets, units),
        grid=(width // depth,),
        in_specs=[pl.BlockSpec((depth, 3 * units), lambda i: (i, 0))] + [whole] * sets,
        out_specs=[whole] * sets,
        out_shape=[jax.ShapeDtypeStruct((rows, width), jnp.bfloat16)] * sets,
        scratch_shapes=[
            pltpu.VMEM((sets * rows, 2 * units), jnp.float32),
            pltpu.VMEM((width, units), jnp.bfloat16),
        ],
        compiler_params=pltpu.CompilerParams(dimension_semantics=("arbitrary",)),
        cost_estimate=pl.CostEstimate(
            flops=6 * sets * rows * width * units, bytes_accessed=6 * width * units, transcendentals=0
        ),
        name="mixer",
    )(weights, *row_sets)


def chip_shift(n_tp, offset):
    return [(t, (t + 2 * offset) % n_tp) for t in range(n_tp)]


def sibling(n_tp):
    return [(t, t ^ 1) for t in range(n_tp)]


def on_device(
    resid,
    query_nope,
    query_rope,
    latent,
    key_rope,
    latent_gain,
    w_key,
    w_value,
    w_out,
    mix_gain,
    w_gate,
    w_up,
    w_down,
):
    n_sp = lax.axis_size("sp")
    n_tp = lax.axis_size("tp")
    rows = query_nope.shape[0]
    here = lax.axis_index("sp")
    upper = here >= n_sp // 2
    first_row = here * rows
    angle = angles((first_row + jnp.arange(rows, dtype=jnp.int32)).astype(jnp.float32), ROPE)

    latent_normed = rms_scale(latent.astype(jnp.float32), latent_gain).astype(jnp.bfloat16)
    key_rotated = rotate(key_rope.astype(jnp.float32), angle).astype(jnp.bfloat16)
    half = rows // 2
    core = lax.axis_index("tp") % 2
    latent_half = lax.dynamic_slice_in_dim(latent_normed, core * half, half, 0)
    rope_quarters = jnp.split(lax.dynamic_slice_in_dim(key_rotated, core * half, half, 0), 4, axis=0)
    packed_rope = jnp.concatenate([rope_quarters[i] for i in (0, 2, 1, 3)], axis=1)
    own_half = jnp.concatenate([latent_half, packed_rope], axis=0)
    mine = lax.all_gather(own_half, "sp", axis=0, tiled=False)
    weights_full = lax.all_gather(
        jnp.concatenate([w_gate, w_up, w_down], axis=1), "sp", axis=0, tiled=True
    )

    here_tp = lax.axis_index("tp")
    chip_pieces = [(0, w_out)] + [(d, lax.ppermute(w_out, "tp", chip_shift(n_tp, d))) for d in (1, 3, 2)]
    owners = []
    for d, _ in chip_pieces:
        owner = (here_tp - 2 * d) % n_tp
        owners += [owner, owner ^ 1]

    rope_query = rotate(
        query_rope.astype(jnp.float32).reshape(rows, 2, ROPE), angle[:, None, :]
    ).astype(jnp.bfloat16)
    blank = jnp.zeros((rows, ROPE), jnp.bfloat16)
    by_head = [
        jnp.concatenate([query_nope[:, h * NOPE : (h + 1) * NOPE], rope_query[:, h], blank], axis=1)
        for h in range(2)
    ]
    kept = jnp.where(upper, by_head[1], by_head[0])
    given = jnp.where(upper, by_head[0], by_head[1])
    partner = [(i, n_sp - 1 - i) for i in range(n_sp)]
    taken = lax.ppermute(given, "sp", partner)
    query_a = jnp.where(
        upper, jnp.concatenate([taken, kept], axis=0), jnp.concatenate([kept, taken], axis=0)
    )
    query_b = jnp.concatenate([query_a[:, :NOPE], query_a[:, NOPE + ROPE :], query_a[:, NOPE : NOPE + ROPE]], axis=1)
    w_kv = jnp.where(
        upper,
        jnp.concatenate([w_key[:, NOPE:], w_value[:, VDIM:]], axis=1),
        jnp.concatenate([w_key[:, :NOPE], w_value[:, :VDIM]], axis=1),
    )
    place = jnp.stack([jnp.minimum(here, n_sp - 1 - here), core] + owners).astype(jnp.int32)
    mine, query_a, query_b, w_kv, place, chip_pieces = lax.optimization_barrier(
        (mine, query_a, query_b, w_kv, place, [w for _, w in chip_pieces])
    )
    theirs = lax.ppermute(mine, "tp", sibling(n_tp))
    out_pieces = [p for w in chip_pieces for p in (w, lax.ppermute(w, "tp", sibling(n_tp)))]
    head_out = attention(place, mine, theirs, query_a, query_b, w_kv)

    groups = [
        [b * n_tp + t for b in (p, n_sp - 1 - p) for t in range(n_tp)] for p in range(n_sp // 2)
    ]
    piece = rows // n_tp
    arrived = lax.all_to_all(
        head_out.reshape(2 * n_tp, piece, VDIM),
        ("sp", "tp"),
        split_axis=0,
        concat_axis=0,
        axis_index_groups=groups,
        tiled=True,
    )
    stream, normed = project(place, arrived, out_pieces, resid, mix_gain)

    def across(rows_now):
        return lax.ppermute(rows_now, "tp", sibling(n_tp))

    def both_cores(rows_mine, from_sibling):
        return rows_mine.astype(jnp.float32) + from_sibling.astype(jnp.float32)

    def home(share, offset):
        return lax.ppermute(share, "tp", chip_shift(n_tp, -offset))

    beside = across(normed)
    after, before, far = (lax.ppermute(normed, "tp", chip_shift(n_tp, d)) for d in (1, 3, 2))
    own_share, own_other = mixer(weights_full, [normed, beside])
    after, before, own_other = lax.optimization_barrier((after, before, own_other))
    own_cross = across(own_other)
    after_share, after_other, before_share, before_other = mixer(
        weights_full, [after, across(after), before, across(before)]
    )
    far, after_other, before_other = lax.optimization_barrier((far, after_other, before_other))
    far_beside = across(far)
    after_sum = both_cores(after_share, across(after_other)).astype(jnp.bfloat16)
    before_sum = both_cores(before_share, across(before_other)).astype(jnp.bfloat16)
    far, far_beside, after_sum, before_sum = lax.optimization_barrier(
        (far, far_beside, after_sum, before_sum)
    )
    shares = [home(after_sum, 1), home(before_sum, 3)]
    far_share, far_other = mixer(weights_full, [far, far_beside])
    shares.append(home(both_cores(far_share, across(far_other)).astype(jnp.bfloat16), 2))
    mixer_out = both_cores(own_share, own_cross)
    for share in shares:
        mixer_out = mixer_out + share.astype(jnp.float32)
    return (stream + 0.5 * mixer_out).astype(jnp.bfloat16)


def solution(mesh):
    return jax.shard_map(
        on_device,
        mesh=mesh,
        in_specs=(
            P(("sp", "tp"), None),
            P("sp", "tp"),
            P("sp", "tp"),
            P("sp", None),
            P("sp", None),
            P(),
            P(None, "tp"),
            P(None, "tp"),
            P("tp", None),
            P(),
            P("sp", "tp"),
            P("sp", "tp"),
            P("sp", "tp"),
        ),
        out_specs=P(("sp", "tp"), None),
        check_vma=False,
    )
```

```python
import functools

import jax
import jax.numpy as jnp
from jax import lax
from jax.experimental import pallas as pl
from jax.experimental.pallas import tpu as pltpu
from jax.sharding import PartitionSpec as P


NOPE = 128
ROPE = 64
VDIM = 128
TILE = 256
LOG2E = 1.4426950408889634

norm_eps = 1e-06
masked_score = -1e30
theta_base = 10000.0


def rotate(values_in, angle):
    half_width = values_in.shape[-1] // 2
    front_half = values_in[..., :half_width]
    back_half = values_in[..., half_width:]
    cosine = jnp.cos(angle)
    sine_part = jnp.sin(angle)
    return jnp.concatenate(
        [front_half * cosine - back_half * sine_part, back_half * cosine + front_half * sine_part],
        axis=-1,
    )


def angles(positions, full_width):
    half_width = full_width // 2
    frequency = theta_base ** (-2.0 * jnp.arange(half_width).astype(jnp.float32) / full_width)
    return positions[:, None] * frequency[None, :]


def rms_scale(values_in, gain):
    return (
        values_in
        * lax.rsqrt(jnp.mean(values_in * values_in, axis=-1, keepdims=True) + norm_eps)
        * gain
    )


def attention_kernel(rows, place_ref, qa_ref, wkv_ref, *refs):
    gathered, (out_ref, buffer_ref, k_ref, v_ref, m_ref, acc_ref, semaphores) = refs[:8], refs[8:]
    step = pl.program_id(0)
    steps = pl.num_programs(0)
    low = place_ref[0]
    core = place_ref[1]
    high = 2 * steps - 1 - low
    half = rows // 2
    scale = (NOPE + ROPE) ** (-0.5) * LOG2E

    def fetch(pair, slot):
        for local in range(2):
            block = 2 * pair + local
            z_back = (place_ref[2] - block // 4) & 3
            y_back = (place_ref[3] - block % 4) & 3
            for side in range(2):
                y_first = core == side
                last = jnp.where(y_first, z_back, y_back)
                first = jnp.where(y_first, y_back, z_back)
                for offset in range(4):

                    @pl.when((last == offset) & (block <= high))
                    def _():
                        pltpu.make_async_copy(
                            gathered[side * 4 + offset].at[first],
                            buffer_ref.at[slot, 2 * local + side],
                            semaphores.at[slot, 2 * local + side],
                        ).start()

    @pl.when(step == 0)
    def _():
        fetch(0, 0)
        m_ref[...] = jnp.full(m_ref.shape, masked_score, jnp.float32)
        acc_ref[...] = jnp.zeros(acc_ref.shape, jnp.float32)
        v_ref[:, :, VDIM:] = jnp.ones((4, half, VDIM), jnp.bfloat16)
        k_ref[:, NOPE + ROPE :, :] = jnp.zeros((4, 256 - NOPE - ROPE, half), jnp.bfloat16)

    @pl.when(step < steps - 1)
    def _():
        fetch(step + 1, (step + 1) % 2)

    def fold(row_start, parts, ahead=None):
        s = [
            jnp.dot(
                qa_ref[pl.ds(row_start, TILE), :], k_ref[part, :, :wide], preferred_element_type=jnp.float32
            )
            for part, wide in parts
        ]
        if ahead is not None:
            wide = parts[-1][1]
            row = lax.broadcasted_iota(jnp.int32, (TILE, wide), 0)
            col = lax.broadcasted_iota(jnp.int32, (TILE, wide), 1)
            s[-1] = jnp.where(col <= row + ahead, s[-1], masked_score)
        old_max = m_ref[pl.ds(row_start, TILE), :]
        new_max = old_max
        for piece in s:
            new_max = jnp.maximum(new_max, jnp.max(piece, axis=-1, keepdims=True) * scale)
        factor = jnp.exp2(old_max - new_max)
        total = jnp.concatenate([factor, factor], axis=1) * acc_ref[pl.ds(row_start, TILE), :]
        for piece, (part, wide) in zip(s, parts):
            wide_max = jnp.concatenate([new_max] * (wide // 128), axis=1)
            weights = jnp.exp2(piece * scale - wide_max).astype(jnp.bfloat16)
            total = total + jnp.dot(weights, v_ref[part, :wide, :], preferred_element_type=jnp.float32)
        m_ref[pl.ds(row_start, TILE), :] = new_max
        acc_ref[pl.ds(row_start, TILE), :] = total

    slot = step % 2
    even = 2 * step
    odd = even + 1

    def expand(local):
        for side in range(2):
            pltpu.make_async_copy(
                gathered[side * 4].at[0],
                buffer_ref.at[slot, 2 * local + side],
                semaphores.at[slot, 2 * local + side],
            ).wait()
        for side in range(2):
            which = 2 * local + (core if side == 0 else 1 - core)
            latent_half = buffer_ref[slot, 2 * local + side, :half, :]
            k_ref[which, :NOPE, :] = lax.dot_general(
                wkv_ref[:, :NOPE], latent_half, (((0,), (1,)), ((), ())), preferred_element_type=jnp.float32
            ).astype(jnp.bfloat16)
            v_ref[which, :, :VDIM] = jnp.dot(
                latent_half, wkv_ref[:, NOPE:], preferred_element_type=jnp.float32
            ).astype(jnp.bfloat16)
            for part in range(2):
                k_ref[which, NOPE : NOPE + ROPE, part * 256 : (part + 1) * 256] = buffer_ref[
                    slot, 2 * local + side, half + part * ROPE : half + (part + 1) * ROPE, :
                ]

    for local in range(2):

        @pl.when(even + local <= high)
        def _(local=local):
            expand(local)

    def whole(group, carry):
        for tile in range(rows // TILE):
            fold(pl.multiple_of(group * rows + tile * TILE, TILE), [(part, half) for part in range(4)])
        return carry

    lax.fori_loop(jnp.where(odd < low, 0, 1), jnp.where(odd < high, 2, 1), whole, 0)

    @pl.when((odd == low) | (odd == high))
    def _():
        base = jnp.where(odd == low, 0, rows)
        for tile in range(rows // TILE):
            fold(pl.multiple_of(base + tile * TILE, TILE), [(0, half), (1, half)])

    at_low = (even == low) | (odd == low)

    @pl.when(at_low | (even == high) | (odd == high))
    def _():
        base = jnp.where(at_low, 0, rows)
        local = jnp.where((even == low) | (even == high), 0, 2)
        for tile, widths in enumerate(([256], [512], [512, 256], [512, 512])):
            parts = [(local + i, wide) for i, wide in enumerate(widths)]
            fold(pl.multiple_of(base + tile * TILE, TILE), parts, widths[-1] - TILE)

    @pl.when(step == steps - 1)
    def _():
        out_ref[...] = (acc_ref[:, :VDIM] / acc_ref[:, VDIM:]).astype(jnp.bfloat16)


def attention(place, gathered, query, w_kv):
    packed_rows, width = gathered[0].shape[1:]
    rows = query.shape[0] // 2
    return pl.pallas_call(
        functools.partial(attention_kernel, rows),
        grid_spec=pltpu.PrefetchScalarGridSpec(
            num_scalar_prefetch=1,
            grid=(8,),
            in_specs=[
                pl.BlockSpec(query.shape, lambda i, place: (0, 0)),
                pl.BlockSpec(w_kv.shape, lambda i, place: (0, 0)),
            ]
            + [pl.BlockSpec(memory_space=pltpu.MemorySpace.HBM)] * len(gathered),
            out_specs=pl.BlockSpec((2 * rows, VDIM), lambda i, place: (0, 0)),
            scratch_shapes=[
                pltpu.VMEM((2, 4, packed_rows, width), jnp.bfloat16),
                pltpu.VMEM((4, 256, rows // 2), jnp.bfloat16),
                pltpu.VMEM((4, rows // 2, 2 * VDIM), jnp.bfloat16),
                pltpu.VMEM((2 * rows, 128), jnp.float32),
                pltpu.VMEM((2 * rows, 2 * VDIM), jnp.float32),
                pltpu.SemaphoreType.DMA((2, 4)),
            ],
        ),
        out_shape=jax.ShapeDtypeStruct((2 * rows, VDIM), jnp.bfloat16),
        compiler_params=pltpu.CompilerParams(dimension_semantics=("arbitrary",)),
        cost_estimate=pl.CostEstimate(
            flops=17 * rows * rows * 1024,
            bytes_accessed=len(gathered) * gathered[0].size * 2,
            transcendentals=17 * rows * rows,
        ),
        name="attention",
    )(place, query, w_kv, *gathered)


def project_kernel(place_ref, heads_ref, *refs):
    count = len(refs) - 4
    pieces, (resid_ref, gain_ref, stream_ref, normed_ref) = refs[:count], refs[count:]
    total = resid_ref[...].astype(jnp.float32)
    for i, piece_ref in enumerate(pieces):
        owner = place_ref[4 + i]
        heads = jnp.concatenate([heads_ref[owner], heads_ref[count + owner]], axis=1)
        total = total + jnp.dot(heads, piece_ref[...], preferred_element_type=jnp.float32)
    stream_ref[...] = total
    square = jnp.mean(total * total, axis=-1, keepdims=True)
    normed_ref[...] = (total * lax.rsqrt(square + norm_eps) * gain_ref[...]).astype(jnp.bfloat16)


def project(place, heads, pieces, resid, gain):
    rows, width = resid.shape
    return pl.pallas_call(
        project_kernel,
        grid_spec=pltpu.PrefetchScalarGridSpec(
            num_scalar_prefetch=1,
            grid=(1,),
            in_specs=[pl.BlockSpec(heads.shape, lambda i, place: (0, 0, 0))]
            + [pl.BlockSpec(p.shape, lambda i, place: (0, 0)) for p in pieces]
            + [
                pl.BlockSpec(resid.shape, lambda i, place: (0, 0)),
                pl.BlockSpec((1, width), lambda i, place: (0, 0)),
            ],
            out_specs=[pl.BlockSpec(resid.shape, lambda i, place: (0, 0))] * 2,
        ),
        out_shape=[
            jax.ShapeDtypeStruct(resid.shape, jnp.float32),
            jax.ShapeDtypeStruct(resid.shape, jnp.bfloat16),
        ],
        cost_estimate=pl.CostEstimate(
            flops=2 * rows * width * width, bytes_accessed=2 * width * width, transcendentals=0
        ),
        name="project",
    )(place, heads, *pieces, resid, gain.reshape(1, width))


def mixer_kernel(sets, units, weight_ref, *refs):
    rows_in, rows_out = refs[:sets], refs[sets : 2 * sets]
    both_ref, down_ref = refs[2 * sets :]
    step = pl.program_id(0)
    depth = weight_ref.shape[0]

    start = pl.multiple_of(step * depth, depth)
    x = jnp.concatenate([r[:, pl.ds(start, depth)] for r in rows_in], axis=0)
    term = jnp.dot(x, weight_ref[:, : 2 * units], preferred_element_type=jnp.float32)

    @pl.when(step == 0)
    def _():
        both_ref[...] = term

    @pl.when(step > 0)
    def _():
        both_ref[...] = both_ref[...] + term

    down_ref[pl.ds(start, depth), :] = weight_ref[:, 2 * units :]

    @pl.when(step == pl.num_programs(0) - 1)
    def _():
        gate = both_ref[:, :units]
        hidden = (gate / (1.0 + jnp.exp(-gate)) * both_ref[:, units:]).astype(jnp.bfloat16)
        out = lax.dot_general(
            hidden, down_ref[...], (((1,), (1,)), ((), ())), preferred_element_type=jnp.float32
        ).astype(jnp.bfloat16)
        rows = out.shape[0] // sets
        for i, ref in enumerate(rows_out):
            ref[...] = out[i * rows : (i + 1) * rows]


def mixer(weights, row_sets):
    rows, width = row_sets[0].shape
    units = weights.shape[1] // 3
    sets = len(row_sets)
    depth = 1024
    whole = pl.BlockSpec((rows, width), lambda i: (0, 0))
    return pl.pallas_call(
        functools.partial(mixer_kernel, sets, units),
        grid=(width // depth,),
        in_specs=[pl.BlockSpec((depth, 3 * units), lambda i: (i, 0))] + [whole] * sets,
        out_specs=[whole] * sets,
        out_shape=[jax.ShapeDtypeStruct((rows, width), jnp.bfloat16)] * sets,
        scratch_shapes=[
            pltpu.VMEM((sets * rows, 2 * units), jnp.float32),
            pltpu.VMEM((width, units), jnp.bfloat16),
        ],
        compiler_params=pltpu.CompilerParams(dimension_semantics=("arbitrary",)),
        cost_estimate=pl.CostEstimate(
            flops=6 * sets * rows * width * units, bytes_accessed=6 * width * units, transcendentals=0
        ),
        name="mixer",
    )(weights, *row_sets)


def chip_shift(n_tp, offset):
    return [(t, (t + 2 * offset) % n_tp) for t in range(n_tp)]


def plane_shift(first, offset):
    pairs = []
    for sp in range(16):
        for tp in range(8):
            z, y = sp // 4, sp % 4
            if (tp % 2 == 0) == first:
                y = (y + offset) % 4
            else:
                z = (z + offset) % 4
            pairs.append((sp * 8 + tp, (z * 4 + y) * 8 + tp))
    return pairs


def sibling(n_tp):
    return [(t, t ^ 1) for t in range(n_tp)]


def on_device(
    resid,
    query_nope,
    query_rope,
    latent,
    key_rope,
    latent_gain,
    w_key,
    w_value,
    w_out,
    mix_gain,
    w_gate,
    w_up,
    w_down,
):
    n_sp = lax.axis_size("sp")
    n_tp = lax.axis_size("tp")
    rows = query_nope.shape[0]
    here = lax.axis_index("sp")
    upper = here >= n_sp // 2
    first_row = here * rows
    angle = angles((first_row + jnp.arange(rows, dtype=jnp.int32)).astype(jnp.float32), ROPE)

    latent_normed = rms_scale(latent.astype(jnp.float32), latent_gain).astype(jnp.bfloat16)
    key_rotated = rotate(key_rope.astype(jnp.float32), angle).astype(jnp.bfloat16)
    half = rows // 2
    core = lax.axis_index("tp") % 2
    latent_half = lax.dynamic_slice_in_dim(latent_normed, core * half, half, 0)
    key_columns = lax.dynamic_slice_in_dim(key_rotated, core * half, half, 0).T
    own_half = jnp.concatenate([latent_half, key_columns[:, :256], key_columns[:, 256:]], axis=0)
    line = [own_half] + [
        lax.ppermute(own_half, ("sp", "tp"), plane_shift(True, d)) for d in (1, 2, 3)
    ]
    line = jnp.stack(line)
    gathered = [line] + [lax.ppermute(line, ("sp", "tp"), plane_shift(False, d)) for d in (1, 2, 3)]
    shard = jnp.concatenate([w_gate, w_up, w_down], axis=1)

    here_tp = lax.axis_index("tp")
    chip_pieces = [(0, w_out)] + [
        (d, lax.ppermute(w_out, "tp", chip_shift(n_tp, d))) for d in (1, 3, 2)
    ]
    owners = []
    for d, _ in chip_pieces:
        owner = (here_tp - 2 * d) % n_tp
        owners += [owner, owner ^ 1]

    rope_query = rotate(
        query_rope.astype(jnp.float32).reshape(rows, 2, ROPE), angle[:, None, :]
    ).astype(jnp.bfloat16)
    by_head = [
        jnp.concatenate(
            [
                query_nope[:, h * NOPE : (h + 1) * NOPE],
                jnp.concatenate([rope_query[:half, h], rope_query[half:, h]], axis=1),
            ],
            axis=0,
        )
        for h in range(2)
    ]
    kept = jnp.where(upper, by_head[1], by_head[0])
    given = jnp.where(upper, by_head[0], by_head[1])
    partner = [(i, n_sp - 1 - i) for i in range(n_sp)]
    taken = lax.ppermute(given, "sp", partner)
    gathered[2], shard = lax.optimization_barrier((gathered[2], shard))
    weights_full = lax.all_gather(shard, "sp", axis=0, tiled=True)
    crossed = []
    for g in gathered:
        crossed.append(lax.ppermute(g, "tp", sibling(n_tp)))
    taken, crossed[0], crossed[1], crossed[3] = lax.optimization_barrier(
        (taken, crossed[0], crossed[1], crossed[3])
    )
    gathered = gathered + crossed
    query_a = jnp.concatenate([jnp.where(upper, taken, kept), jnp.where(upper, kept, taken)], axis=0)
    query_a = query_a.reshape(2, rows + half, NOPE)
    rope_part = jnp.concatenate([query_a[:, rows:, :ROPE], query_a[:, rows:, ROPE:]], axis=1)
    query_a = jnp.concatenate([query_a[:, :rows], rope_part, jnp.zeros_like(rope_part)], axis=2)
    query_a = query_a.reshape(2 * rows, 2 * NOPE)
    w_kv = jnp.where(
        upper,
        jnp.concatenate([w_key[:, NOPE:], w_value[:, VDIM:]], axis=1),
        jnp.concatenate([w_key[:, :NOPE], w_value[:, :VDIM]], axis=1),
    )
    place = jnp.stack([jnp.minimum(here, n_sp - 1 - here), core, here // 4, here % 4] + owners).astype(jnp.int32)
    head_out = attention(place, gathered, query_a, w_kv)
    out_pieces = [p for _, w in chip_pieces for p in (w, lax.ppermute(w, "tp", sibling(n_tp)))]

    groups = [
        [b * n_tp + t for b in (p, n_sp - 1 - p) for t in range(n_tp)] for p in range(n_sp // 2)
    ]
    piece = rows // n_tp
    arrived = lax.all_to_all(
        head_out.reshape(2 * n_tp, piece, VDIM),
        ("sp", "tp"),
        split_axis=0,
        concat_axis=0,
        axis_index_groups=groups,
        tiled=True,
    )
    stream, normed = project(place, arrived, out_pieces, resid, mix_gain)

    def across(rows_now):
        return lax.ppermute(rows_now, "tp", sibling(n_tp))

    def both_cores(rows_mine, from_sibling):
        return rows_mine.astype(jnp.float32) + from_sibling.astype(jnp.float32)

    def home(share, offset):
        return lax.ppermute(share, "tp", chip_shift(n_tp, -offset))

    beside = across(normed)
    after, before, far = (lax.ppermute(normed, "tp", chip_shift(n_tp, d)) for d in (1, 3, 2))
    own_share, own_other = mixer(weights_full, [normed, beside])
    after, before, own_other = lax.optimization_barrier((after, before, own_other))
    own_cross = across(own_other)
    after_share, after_other, before_share, before_other = mixer(
        weights_full, [after, across(after), before, across(before)]
    )
    far, after_other, before_other = lax.optimization_barrier((far, after_other, before_other))
    far_beside = across(far)
    after_sum = both_cores(after_share, across(after_other)).astype(jnp.bfloat16)
    before_sum = both_cores(before_share, across(before_other)).astype(jnp.bfloat16)
    far, far_beside, after_sum, before_sum = lax.optimization_barrier(
        (far, far_beside, after_sum, before_sum)
    )
    shares = [home(after_sum, 1)]
    shares.append(home(before_sum, 3))
    far_share, far_other = mixer(weights_full, [far, far_beside])
    shares.append(home(both_cores(far_share, across(far_other)).astype(jnp.bfloat16), 2))
    mixer_out = both_cores(own_share, own_cross)
    for share in shares:
        mixer_out = mixer_out + share.astype(jnp.float32)
    return (stream + 0.5 * mixer_out).astype(jnp.bfloat16)


def solution(mesh):
    return jax.shard_map(
        on_device,
        mesh=mesh,
        in_specs=(
            P(("sp", "tp"), None),
            P("sp", "tp"),
            P("sp", "tp"),
            P("sp", None),
            P("sp", None),
            P(),
            P(None, "tp"),
            P(None, "tp"),
            P("tp", None),
            P(),
            P("sp", "tp"),
            P("sp", "tp"),
            P("sp", "tp"),
        ),
        out_specs=P(("sp", "tp"), None),
        check_vma=False,
    )
```

```python
import functools

import jax
import jax.numpy as jnp
from jax import lax
from jax.experimental import pallas as pl
from jax.experimental.pallas import tpu as pltpu
from jax.sharding import PartitionSpec as P


NOPE = 128
ROPE = 64
VDIM = 128
TILE = 256
LOG2E = 1.4426950408889634

norm_eps = 1e-06
masked_score = -1e30
theta_base = 10000.0


def rotate(values_in, angle):
    half_width = values_in.shape[-1] // 2
    front_half = values_in[..., :half_width]
    back_half = values_in[..., half_width:]
    cosine = jnp.cos(angle)
    sine_part = jnp.sin(angle)
    return jnp.concatenate(
        [front_half * cosine - back_half * sine_part, back_half * cosine + front_half * sine_part],
        axis=-1,
    )


def angles(positions, full_width):
    half_width = full_width // 2
    frequency = theta_base ** (-2.0 * jnp.arange(half_width).astype(jnp.float32) / full_width)
    return positions[:, None] * frequency[None, :]


def rms_scale(values_in, gain):
    return (
        values_in
        * lax.rsqrt(jnp.mean(values_in * values_in, axis=-1, keepdims=True) + norm_eps)
        * gain
    )


def attention_kernel(rows, place_ref, qa_ref, wkv_ref, *refs):
    gathered, (out_ref, buffer_ref, k_ref, v_ref, m_ref, acc_ref, semaphores) = refs[:8], refs[8:]
    step = pl.program_id(0)
    steps = pl.num_programs(0)
    low = place_ref[0]
    core = place_ref[1]
    high = 2 * steps - 1 - low
    half = rows // 2
    scale = (NOPE + ROPE) ** (-0.5) * LOG2E

    def fetch(pair, slot):
        for local in range(2):
            block = 2 * pair + local
            z_back = (place_ref[2] - block // 4) & 3
            y_back = (place_ref[3] - block % 4) & 3
            for side in range(2):
                y_first = core == side
                last = jnp.where(y_first, z_back, y_back)
                first = jnp.where(y_first, y_back, z_back)
                for offset in range(4):

                    @pl.when((last == offset) & (block <= high))
                    def _():
                        pltpu.make_async_copy(
                            gathered[side * 4 + offset].at[first],
                            buffer_ref.at[slot, 2 * local + side],
                            semaphores.at[slot, 2 * local + side],
                        ).start()

    @pl.when(step == 0)
    def _():
        fetch(0, 0)

        def clear(tile, carry):
            at = pl.ds(pl.multiple_of(tile * TILE, TILE), TILE)
            m_ref[at, :] = jnp.full((TILE, 128), masked_score, jnp.float32)
            acc_ref[at, :] = jnp.zeros((TILE, 2 * VDIM), jnp.float32)
            return carry

        lax.fori_loop(0, 2 * rows // TILE, clear, 0)

        def pad(part, carry):
            v_ref[part, :, VDIM:] = jnp.ones((half, VDIM), jnp.bfloat16)
            k_ref[part, NOPE + ROPE :, :] = jnp.zeros((256 - NOPE - ROPE, half), jnp.bfloat16)
            return carry

        lax.fori_loop(0, 4, pad, 0)

    @pl.when(step < steps - 1)
    def _():
        fetch(step + 1, (step + 1) % 2)

    def fold(row_start, parts, ahead=None):
        s = [
            jnp.dot(
                qa_ref[pl.ds(row_start, TILE), :], k_ref[part, :, :wide], preferred_element_type=jnp.float32
            )
            for part, wide in parts
        ]
        if ahead is not None:
            wide = parts[-1][1]
            row = lax.broadcasted_iota(jnp.int32, (TILE, wide), 0)
            col = lax.broadcasted_iota(jnp.int32, (TILE, wide), 1)
            s[-1] = jnp.where(col <= row + ahead, s[-1], masked_score)
        old_max = m_ref[pl.ds(row_start, TILE), :]
        new_max = old_max
        for piece in s:
            new_max = jnp.maximum(new_max, jnp.max(piece, axis=-1, keepdims=True) * scale)
        factor = jnp.exp2(old_max - new_max)
        total = jnp.concatenate([factor, factor], axis=1) * acc_ref[pl.ds(row_start, TILE), :]
        for piece, (part, wide) in zip(s, parts):
            wide_max = jnp.concatenate([new_max] * (wide // 128), axis=1)
            weights = jnp.exp2(piece * scale - wide_max).astype(jnp.bfloat16)
            total = total + jnp.dot(weights, v_ref[part, :wide, :], preferred_element_type=jnp.float32)
        m_ref[pl.ds(row_start, TILE), :] = new_max
        acc_ref[pl.ds(row_start, TILE), :] = total

    slot = step % 2
    even = 2 * step
    odd = even + 1

    def expand(local):
        for side in range(2):
            pltpu.make_async_copy(
                gathered[side * 4].at[0],
                buffer_ref.at[slot, 2 * local + side],
                semaphores.at[slot, 2 * local + side],
            ).wait()
        for side in range(2):
            which = 2 * local + (core if side == 0 else 1 - core)
            latent_half = buffer_ref[slot, 2 * local + side, :half, :]
            k_ref[which, :NOPE, :] = lax.dot_general(
                wkv_ref[:, :NOPE], latent_half, (((0,), (1,)), ((), ())), preferred_element_type=jnp.float32
            ).astype(jnp.bfloat16)
            v_ref[which, :, :VDIM] = jnp.dot(
                latent_half, wkv_ref[:, NOPE:], preferred_element_type=jnp.float32
            ).astype(jnp.bfloat16)
            for part in range(2):
                k_ref[which, NOPE : NOPE + ROPE, part * 256 : (part + 1) * 256] = buffer_ref[
                    slot, 2 * local + side, half + part * ROPE : half + (part + 1) * ROPE, :
                ]

    for local in range(2):

        @pl.when(even + local <= high)
        def _(local=local):
            expand(local)

    def whole(group, carry):
        for tile in range(rows // TILE):
            fold(pl.multiple_of(group * rows + tile * TILE, TILE), [(part, half) for part in range(4)])
        return carry

    lax.fori_loop(jnp.where(odd < low, 0, 1), jnp.where(odd < high, 2, 1), whole, 0)

    @pl.when((odd == low) | (odd == high))
    def _():
        base = jnp.where(odd == low, 0, rows)

        def two_tiles(pair, carry):
            for tile in range(2):
                fold(pl.multiple_of(base + (2 * pair + tile) * TILE, TILE), [(0, half), (1, half)])
            return carry

        lax.fori_loop(0, rows // TILE // 2, two_tiles, 0)

    at_low = (even == low) | (odd == low)

    @pl.when(at_low | (even == high) | (odd == high))
    def _():
        base = jnp.where(at_low, 0, rows)
        local = jnp.where((even == low) | (even == high), 0, 2)
        for tile, widths in enumerate(([256], [512], [512, 256], [512, 512])):
            parts = [(local + i, wide) for i, wide in enumerate(widths)]
            fold(pl.multiple_of(base + tile * TILE, TILE), parts, widths[-1] - TILE)

    @pl.when(step == steps - 1)
    def _():

        def finish(tile, carry):
            at = pl.ds(pl.multiple_of(tile * TILE, TILE), TILE)
            out_ref[at, :] = (acc_ref[at, :VDIM] / acc_ref[at, VDIM:]).astype(jnp.bfloat16)
            return carry

        lax.fori_loop(0, 2 * rows // TILE, finish, 0)


def attention(place, gathered, query, w_kv):
    packed_rows, width = gathered[0].shape[1:]
    rows = query.shape[0] // 2
    return pl.pallas_call(
        functools.partial(attention_kernel, rows),
        grid_spec=pltpu.PrefetchScalarGridSpec(
            num_scalar_prefetch=1,
            grid=(8,),
            in_specs=[
                pl.BlockSpec(query.shape, lambda i, place: (0, 0)),
                pl.BlockSpec(w_kv.shape, lambda i, place: (0, 0)),
            ]
            + [pl.BlockSpec(memory_space=pltpu.MemorySpace.HBM)] * len(gathered),
            out_specs=pl.BlockSpec((2 * rows, VDIM), lambda i, place: (0, 0)),
            scratch_shapes=[
                pltpu.VMEM((2, 4, packed_rows, width), jnp.bfloat16),
                pltpu.VMEM((4, 256, rows // 2), jnp.bfloat16),
                pltpu.VMEM((4, rows // 2, 2 * VDIM), jnp.bfloat16),
                pltpu.VMEM((2 * rows, 128), jnp.float32),
                pltpu.VMEM((2 * rows, 2 * VDIM), jnp.float32),
                pltpu.SemaphoreType.DMA((2, 4)),
            ],
        ),
        out_shape=jax.ShapeDtypeStruct((2 * rows, VDIM), jnp.bfloat16),
        compiler_params=pltpu.CompilerParams(
            dimension_semantics=("arbitrary",), vmem_limit_bytes=24 * 2**20
        ),
        cost_estimate=pl.CostEstimate(
            flops=17 * rows * rows * 1024,
            bytes_accessed=len(gathered) * gathered[0].size * 2,
            transcendentals=17 * rows * rows,
        ),
        name="attention",
    )(place, query, w_kv, *gathered)


def project_kernel(place_ref, heads_ref, resid_ref, gain_ref, *refs):
    pieces, (stream_ref, normed_ref) = refs[:-2], refs[-2:]
    count = len(pieces)
    total = resid_ref[...].astype(jnp.float32)
    for i, piece_ref in enumerate(pieces):
        owner = place_ref[4 + i]
        heads = jnp.concatenate([heads_ref[owner], heads_ref[count + owner]], axis=1)
        total = total + jnp.dot(heads, piece_ref[...], preferred_element_type=jnp.float32)
    stream_ref[...] = total
    square = jnp.mean(total * total, axis=-1, keepdims=True)
    normed_ref[...] = (total * lax.rsqrt(square + norm_eps) * gain_ref[...]).astype(jnp.bfloat16)


def project(place, heads, pieces, resid, gain):
    rows, width = resid.shape
    in_vmem = pl.BlockSpec(memory_space=pltpu.MemorySpace.VMEM)
    return pl.pallas_call(
        project_kernel,
        in_specs=[pl.BlockSpec(memory_space=pltpu.MemorySpace.SMEM)] + [in_vmem] * (3 + len(pieces)),
        out_specs=[in_vmem] * 2,
        out_shape=[
            jax.ShapeDtypeStruct(resid.shape, jnp.float32),
            jax.ShapeDtypeStruct(resid.shape, jnp.bfloat16),
        ],
        compiler_params=pltpu.CompilerParams(vmem_limit_bytes=24 * 2**20),
        cost_estimate=pl.CostEstimate(
            flops=2 * rows * width * width, bytes_accessed=2 * width * width, transcendentals=0
        ),
        name="project",
    )(place, heads, resid, gain.reshape(1, width), *pieces)


def mixer_kernel(sets, units, weight_ref, *refs):
    rows_in, rows_out = refs[:sets], refs[sets:]
    x = jnp.concatenate([r[...] for r in rows_in], axis=0)
    both = jnp.dot(x, weight_ref[:, : 2 * units], preferred_element_type=jnp.float32)
    gate = both[:, :units]
    hidden = (gate / (1.0 + jnp.exp(-gate)) * both[:, units:]).astype(jnp.bfloat16)
    out = lax.dot_general(
        hidden, weight_ref[:, 2 * units :], (((1,), (1,)), ((), ())), preferred_element_type=jnp.float32
    ).astype(jnp.bfloat16)
    rows = out.shape[0] // sets
    for i, ref in enumerate(rows_out):
        ref[...] = out[i * rows : (i + 1) * rows]


def mixer(weights, row_sets):
    rows, width = row_sets[0].shape
    units = weights.shape[1] // 3
    sets = len(row_sets)
    in_vmem = pl.BlockSpec(memory_space=pltpu.MemorySpace.VMEM)
    return pl.pallas_call(
        functools.partial(mixer_kernel, sets, units),
        in_specs=[in_vmem] * (1 + sets),
        out_specs=[in_vmem] * sets,
        out_shape=[jax.ShapeDtypeStruct((rows, width), jnp.bfloat16)] * sets,
        compiler_params=pltpu.CompilerParams(vmem_limit_bytes=32 * 2**20),
        cost_estimate=pl.CostEstimate(
            flops=6 * sets * rows * width * units, bytes_accessed=6 * width * units, transcendentals=0
        ),
        name="mixer",
    )(weights, *row_sets)


def chip_shift(n_tp, offset):
    return [(t, (t + 2 * offset) % n_tp) for t in range(n_tp)]


def plane_shift(first, offset):
    pairs = []
    for sp in range(16):
        for tp in range(8):
            z, y = sp // 4, sp % 4
            if (tp % 2 == 0) == first:
                y = (y + offset) % 4
            else:
                z = (z + offset) % 4
            pairs.append((sp * 8 + tp, (z * 4 + y) * 8 + tp))
    return pairs


def sibling(n_tp):
    return [(t, t ^ 1) for t in range(n_tp)]


def on_device(
    resid,
    query_nope,
    query_rope,
    latent,
    key_rope,
    latent_gain,
    w_key,
    w_value,
    w_out,
    mix_gain,
    w_gate,
    w_up,
    w_down,
):
    n_sp = lax.axis_size("sp")
    n_tp = lax.axis_size("tp")
    rows = query_nope.shape[0]
    here = lax.axis_index("sp")
    upper = here >= n_sp // 2
    first_row = here * rows
    angle = angles((first_row + jnp.arange(rows, dtype=jnp.int32)).astype(jnp.float32), ROPE)

    latent_normed = rms_scale(latent.astype(jnp.float32), latent_gain).astype(jnp.bfloat16)
    key_rotated = rotate(key_rope.astype(jnp.float32), angle).astype(jnp.bfloat16)
    half = rows // 2
    core = lax.axis_index("tp") % 2
    latent_half = lax.dynamic_slice_in_dim(latent_normed, core * half, half, 0)
    key_columns = lax.dynamic_slice_in_dim(key_rotated, core * half, half, 0).T
    own_half = jnp.concatenate([latent_half, key_columns[:, :256], key_columns[:, 256:]], axis=0)
    line = [own_half] + [
        lax.ppermute(own_half, ("sp", "tp"), plane_shift(True, d)) for d in (1, 2, 3)
    ]
    line = jnp.stack(line)
    gathered = [line] + [
        lax.ppermute(line, ("sp", "tp"), plane_shift(False, d)) for d in (1, 2, 3)
    ]
    shard = jnp.concatenate([w_gate, w_up, w_down], axis=1)

    here_tp = lax.axis_index("tp")
    chip_pieces = [(0, w_out)] + [
        (d, lax.ppermute(w_out, "tp", chip_shift(n_tp, d))) for d in (1, 3, 2)
    ]
    owners = []
    for d, _ in chip_pieces:
        owner = (here_tp - 2 * d) % n_tp
        owners += [owner, owner ^ 1]

    rope_query = rotate(
        query_rope.astype(jnp.float32).reshape(rows, 2, ROPE), angle[:, None, :]
    ).astype(jnp.bfloat16)
    by_head = [
        jnp.concatenate(
            [
                query_nope[:, h * NOPE : (h + 1) * NOPE],
                jnp.concatenate([rope_query[:half, h], rope_query[half:, h]], axis=1),
            ],
            axis=0,
        )
        for h in range(2)
    ]
    kept = jnp.where(upper, by_head[1], by_head[0])
    given = jnp.where(upper, by_head[0], by_head[1])
    partner = [(i, n_sp - 1 - i) for i in range(n_sp)]
    taken = lax.ppermute(given, "sp", partner)
    gathered[1], gathered[3], shard = lax.optimization_barrier((gathered[1], gathered[3], shard))
    weights_full = lax.all_gather(shard, "sp", axis=0, tiled=True)
    crossed = []
    for g in gathered:
        crossed.append(lax.ppermute(g, "tp", sibling(n_tp)))
    taken, crossed[0], crossed[1], crossed[3] = lax.optimization_barrier(
        (taken, crossed[0], crossed[1], crossed[3])
    )
    gathered = gathered + crossed
    query_a = jnp.concatenate([jnp.where(upper, taken, kept), jnp.where(upper, kept, taken)], axis=0)
    query_a = query_a.reshape(2, rows + half, NOPE)
    rope_part = jnp.concatenate([query_a[:, rows:, :ROPE], query_a[:, rows:, ROPE:]], axis=1)
    query_a = jnp.concatenate([query_a[:, :rows], rope_part, jnp.zeros_like(rope_part)], axis=2)
    query_a = query_a.reshape(2 * rows, 2 * NOPE)
    w_kv = jnp.where(
        upper,
        jnp.concatenate([w_key[:, NOPE:], w_value[:, VDIM:]], axis=1),
        jnp.concatenate([w_key[:, :NOPE], w_value[:, :VDIM]], axis=1),
    )
    place = jnp.stack([jnp.minimum(here, n_sp - 1 - here), core, here // 4, here % 4] + owners).astype(jnp.int32)
    head_out = attention(place, gathered, query_a, w_kv)
    out_pieces = [p for _, w in chip_pieces for p in (w, lax.ppermute(w, "tp", sibling(n_tp)))]

    groups = [
        [b * n_tp + t for b in (p, n_sp - 1 - p) for t in range(n_tp)] for p in range(n_sp // 2)
    ]
    piece = rows // n_tp
    arrived = lax.all_to_all(
        head_out.reshape(2 * n_tp, piece, VDIM),
        ("sp", "tp"),
        split_axis=0,
        concat_axis=0,
        axis_index_groups=groups,
        tiled=True,
    )
    stream, normed = project(place, arrived, out_pieces, resid, mix_gain)

    def across(rows_now):
        return lax.ppermute(rows_now, "tp", sibling(n_tp))

    def both_cores(rows_mine, from_sibling):
        return rows_mine.astype(jnp.float32) + from_sibling.astype(jnp.float32)

    def home(share, offset):
        return lax.ppermute(share, "tp", chip_shift(n_tp, -offset))

    beside = across(normed)
    after, before = (lax.ppermute(normed, "tp", chip_shift(n_tp, d)) for d in (1, 3))
    far_halves = [
        lax.ppermute(after[: piece // 2], "tp", chip_shift(n_tp, 1)),
        lax.ppermute(before[piece // 2 :], "tp", chip_shift(n_tp, 3)),
    ]
    far = jnp.concatenate(far_halves, axis=0)
    own_share, own_other = mixer(weights_full, [normed, beside])
    after, before, own_other = lax.optimization_barrier((after, before, own_other))
    own_cross = across(own_other)
    near_rows = [after, across(after), before, across(before)]
    after_share, after_other, before_share, before_other = mixer(weights_full, near_rows)
    after_sum = both_cores(after_share, across(after_other)).astype(jnp.bfloat16)
    before_sum = both_cores(before_share, across(before_other)).astype(jnp.bfloat16)
    shares = [home(after_sum, 1)]
    shares.append(home(before_sum, 3))
    far_beside = across(far)
    far_share, far_other = mixer(weights_full, [far, far_beside])
    shares.append(home(both_cores(far_share, across(far_other)).astype(jnp.bfloat16), 2))
    mixer_out = both_cores(own_share, own_cross)
    for share in shares:
        mixer_out = mixer_out + share.astype(jnp.float32)
    return (stream + 0.5 * mixer_out).astype(jnp.bfloat16)


def solution(mesh):
    return jax.shard_map(
        on_device,
        mesh=mesh,
        in_specs=(
            P(("sp", "tp"), None),
            P("sp", "tp"),
            P("sp", "tp"),
            P("sp", None),
            P("sp", None),
            P(),
            P(None, "tp"),
            P(None, "tp"),
            P("tp", None),
            P(),
            P("sp", "tp"),
            P("sp", "tp"),
            P("sp", "tp"),
        ),
        out_specs=P(("sp", "tp"), None),
        check_vma=False,
    )
```
